32 devices in a mesh: ep: 4 (over y, x), tp: 8 (over z, core).
Axes of the slice: x: 2, y: 2, z: 4, core: 2. Of those that a mesh axis runs over, the one named last changes fastest.
Arguments:
- hidden_in: bfloat16 [128, 4096], P('ep'), may hold values from -6 to 6
- mix_gain: float32 [4096], replicated, may hold values from 0.1 to 1.9
- w_query: bfloat16 [4096, 2048], P('ep', 'tp'), may hold values from -0.09375 to 0.09375
- w_key: bfloat16 [4096, 2048], P('ep', 'tp'), may hold values from -0.09375 to 0.09375
- w_value: bfloat16 [4096, 2048], P('ep', 'tp'), may hold values from -0.09375 to 0.09375
- w_outgate: bfloat16 [4096, 2048], P('ep', 'tp'), may hold values from -0.09375 to 0.09375
- w_gates: bfloat16 [2, 4096, 32], P(None, None, 'tp'), may hold values from -0.09375 to 0.09375
- gate_bias: float32 [2, 32], P(None, 'tp'), may hold values from -1 to 4
- state_matrix: float32 [128, 32, 64, 64], P('ep', 'tp'), may hold values from -2 to 2
- state_norm: float32 [128, 32, 64], P('ep', 'tp'), may hold values from -2 to 2
- state_max: float32 [128, 32], P('ep', 'tp'), may hold values from -3 to 3
- w_mix_out: bfloat16 [2048, 4096], P('tp'), may hold values from -0.125 to 0.125
- ffn_gain: float32 [4096], replicated, may hold values from 0.1 to 1.9
- routes: int32 [128, 2], replicated, may hold values from 0 to 7, all different within a row; in each aligned block of 32 rows (0 to 31, 32 to 63, ...) at most 9 rows name the same one
- route_weights: float32 [128, 2], P('ep'), may hold values from 0.1 to 1
- expert_gate: bfloat16 [8, 4096, 2048], P('ep', None, 'tp'), may hold values from -0.09375 to 0.09375
- expert_up: bfloat16 [8, 4096, 2048], P('ep', None, 'tp'), may hold values from -0.09375 to 0.09375
- expert_down: bfloat16 [8, 2048, 4096], P('ep', 'tp'), may hold values from -0.125 to 0.125
- shared_gate: bfloat16 [4096, 1024], P(None, 'tp'), may hold values from -0.09375 to 0.09375
- shared_up: bfloat16 [4096, 1024], P(None, 'tp'), may hold values from -0.09375 to 0.09375
- shared_down: bfloat16 [1024, 4096], P('tp'), may hold values from -0.1875 to 0.1875
Outputs:
- result: bfloat16 [128, 4096], P('ep', 'tp')
- new_matrix: float32 [128, 32, 64, 64], P('ep', 'tp')
- new_norm: float32 [128, 32, 64], P('ep', 'tp')
- new_max: float32 [128, 32], P('ep', 'tp')
The draws below stay inside these ranges and needn't reach their ends.
Inputs may be any that keep to these rules, and one draw needn't show every extreme that they name: `routes`: each row names 2 different experts. In each aligned block of 32 rows (the rows of one device group along ep) no expert is named by more than 9 rows, a bound that some block reaches.
All inputs are finite; a program needn't handle non-finite values.
Results may differ from the reference program's by a relative error of at most 0.023.
Values may be sent and summed in bfloat16 or wider, within the bound.
No kernel may reach another device: no remote copies, remote signals or barrier semaphores. Data moves between devices by JAX's collectives and lax.ppermute only.
A program may use at most 64 MiB of HBM per device.

```python
import math
import jax
import jax.numpy as jnp
import numpy as np
from jax import lax

D = 4096
HEADS = 32
HEAD_DIM = 64
EXPERT_WIDTH = 2048
SHARED_WIDTH = 1024
TOP = 2
SEQ_GRP = 32
M_WIDTH = 2048
EXPERTS = 8
CAP = 9
BATCH = 128
N_EP = 4
N_TP = 8


def block_scale(own_key, shape, cuts, least, top_value):
    gain = 1.0
    for axis_at, parts in cuts:
        heights = jax.random.uniform(jax.random.fold_in(jax.random.fold_in(own_key, 6), axis_at), (parts,), jnp.float32, least / len(cuts), top_value / len(cuts))
        gain = gain * jnp.repeat(jnp.exp(heights), shape[axis_at] // parts).reshape((-1,) + (1,) * (len(shape) - 1 - axis_at))
    return gain


def deal_out(key, own, number, rows, count, top, most, skew):
    sequence = jax.random.permutation(key, count)
    packed, ordinary = portions_of(count, rows * top, most, skew, True), portions_of(count, rows * top, most, skew, False)
    places = jnp.arange(count)

    def named(lengths, rotation):
        used = int((lengths > 0).sum())
        fixed = max(1, used // 4)
        shifted = fixed + (places - fixed + rotation * (used - fixed)) % max(1, count - fixed)
        return jnp.zeros((count,), jnp.int32).at[sequence[jnp.where(places < fixed, places, shifted)]].set(jnp.asarray(lengths, jnp.int32))

    lengths = jnp.where(number % 4 == 0, named(packed, number // 4), named(ordinary, number - number // 4 - 1))
    mixed = jax.random.permutation(jax.random.fold_in(own, 3), count)
    source_of, receiver = mixed[0:count // 2 * 2:2], mixed[1:count // 2 * 2:2]
    room = jnp.minimum(lengths[source_of] - 1, most - lengths[receiver]) // 2
    room = jnp.where((source_of == sequence[0]) | (receiver == sequence[0]) | (lengths[receiver] == 0), 0, jnp.maximum(room, 0))
    shifted = jax.random.randint(jax.random.fold_in(own, 4), (count // 2,), 0, 1 << 20) % (room + 1)
    lengths = lengths.at[source_of].add(-shifted).at[receiver].add(shifted)
    items = jnp.searchsorted(jnp.cumsum(lengths), jnp.arange(rows * top), side="right").astype(jnp.int32)
    table = items.reshape(top, rows).T
    table = table[jax.random.permutation(jax.random.fold_in(own, 1), rows)]
    rotation = jax.random.randint(jax.random.fold_in(own, 2), (rows, 1), 0, top)
    return jnp.take_along_axis(table, (jnp.arange(top)[None, :] + rotation) % top, axis=1)


def portions_of(number_of, total, reach, lean, full):
    portions = [(1 << 20) // math.isqrt(standing ** lean) + 1 for standing in range(1, number_of + 1)]
    largest = reach if full else min(reach, max(-(-total // number_of), total * portions[0] // sum(portions)))
    least = 1 if total - largest >= number_of - 1 else 0
    holding, surplus = [largest] + [least] * (number_of - 1), total - largest - least * (number_of - 1)
    while surplus > 0:
        movable = [i for i in range(1, number_of) if holding[i] < largest] or [i for i in range(1, number_of) if holding[i] < reach]
        pool, left = sum([portions[i] for i in movable]), surplus
        for i in movable:
            addition = min(reach - holding[i], max(1, left * portions[i] // pool), surplus)
            holding[i] = holding[i] + addition
            surplus = surplus - addition
    return np.array(holding)


def bell_draw(rng, extent, scale, reach, cuts=(), kind=jnp.bfloat16):
    level = block_scale(rng, extent, cuts, -0.22, 0.18) if cuts else 1.0
    values = jax.random.normal(rng, extent, jnp.float32) * scale * level
    return jnp.minimum(jnp.maximum(values, -reach), reach).astype(kind)


def setup_inputs(seed: int = 0) -> dict:
    streams_of = jax.random.split(jax.random.key(seed), 22)
    hidden_in = bell_draw(streams_of[0], (BATCH, D), 1.0, 6.0, ((0, 4),))
    mix_gain = jnp.clip(1.0 + 0.18 * jax.random.normal(streams_of[1], (D,), jnp.float32), 0.1, 1.9)
    w_query = bell_draw(streams_of[2], (D, M_WIDTH), D ** -0.5, 0.09375, ((0, 4), (1, 8)))
    w_key = bell_draw(streams_of[3], (D, M_WIDTH), D ** -0.5, 0.09375, ((0, 4), (1, 8)))
    w_value = bell_draw(streams_of[4], (D, M_WIDTH), D ** -0.5, 0.09375, ((0, 4), (1, 8)))
    w_outgate = bell_draw(streams_of[5], (D, M_WIDTH), D ** -0.5, 0.09375, ((0, 4), (1, 8)))
    w_gates = bell_draw(streams_of[6], (2, D, HEADS), D ** -0.5, 0.09375, ((2, 8),))
    gate_bias = jnp.clip(-1.0 + 5.0 * jax.random.uniform(streams_of[7], (2, HEADS), jnp.float32) ** block_scale(streams_of[7], (2, HEADS), ((1, 8),), -0.2, 0.2), -1.0, 4.0)
    state_matrix = bell_draw(streams_of[8], (BATCH, HEADS, HEAD_DIM, HEAD_DIM), 0.15, 2.0, ((0, 4), (1, 8)), jnp.float32)
    state_norm = bell_draw(streams_of[9], (BATCH, HEADS, HEAD_DIM), 0.15, 2.0, ((0, 4), (1, 8)), jnp.float32)
    state_max = jnp.clip(jax.random.uniform(streams_of[10], (BATCH, HEADS), jnp.float32, -3.0, 3.0) * block_scale(streams_of[10], (BATCH, HEADS), ((0, 4), (1, 8)), -0.4, 0.0), -3.0, 3.0)
    w_mix_out = bell_draw(streams_of[11], (M_WIDTH, D), M_WIDTH ** -0.5, 0.125, ((0, 8),))
    ffn_gain = jnp.clip(1.0 + 0.18 * jax.random.normal(streams_of[12], (D,), jnp.float32), 0.1, 1.9)
    routes_keys = jax.random.split(jax.random.fold_in(streams_of[13], 1), BATCH // SEQ_GRP)
    routes_turns = jax.random.permutation(jax.random.fold_in(streams_of[13], 3), BATCH // SEQ_GRP)
    routes = jax.vmap(lambda own, number: deal_out(jax.random.fold_in(streams_of[13], 2), own, number, SEQ_GRP, EXPERTS, TOP, CAP, 2))(routes_keys, routes_turns).reshape((BATCH, TOP))
    route_weights = jnp.clip(jnp.exp(math.log(1.0) - 2.3025851 * jax.random.uniform(streams_of[14], (BATCH, TOP), jnp.float32) ** block_scale(streams_of[14], (BATCH, TOP), ((0, 4),), -0.2, 0.2)), 0.1, 1.0)
    expert_gate = bell_draw(streams_of[15], (EXPERTS, D, EXPERT_WIDTH), D ** -0.5, 0.09375, ((0, 4), (2, 8)))
    expert_up = bell_draw(streams_of[16], (EXPERTS, D, EXPERT_WIDTH), D ** -0.5, 0.09375, ((0, 4), (2, 8)))
    expert_down = bell_draw(streams_of[17], (EXPERTS, EXPERT_WIDTH, D), EXPERT_WIDTH ** -0.5, 0.125, ((0, 4), (1, 8)))
    shared_gate = bell_draw(streams_of[18], (D, SHARED_WIDTH), D ** -0.5, 0.09375, ((1, 8),))
    shared_up = bell_draw(streams_of[19], (D, SHARED_WIDTH), D ** -0.5, 0.09375, ((1, 8),))
    shared_down = bell_draw(streams_of[20], (SHARED_WIDTH, D), SHARED_WIDTH ** -0.5, 0.1875, ((0, 8),))
    return dict(hidden_in=hidden_in, mix_gain=mix_gain, w_query=w_query, w_key=w_key, w_value=w_value, w_outgate=w_outgate, w_gates=w_gates, gate_bias=gate_bias, state_matrix=state_matrix, state_norm=state_norm, state_max=state_max, w_mix_out=w_mix_out, ffn_gain=ffn_gain, routes=routes, route_weights=route_weights, expert_gate=expert_gate, expert_up=expert_up, expert_down=expert_down, shared_gate=shared_gate, shared_up=shared_up, shared_down=shared_down)


norm_eps = 1e-06

def rms_scale(inputs, scales):
    floats = inputs.astype(jnp.float32)
    return floats * lax.rsqrt(lax.optimization_barrier(jnp.mean(floats * floats, -1, keepdims=True)) + norm_eps) * scales

def block_sum(hidden, down_weight):
    row_count = hidden.shape[0]
    unit_count = hidden.shape[1]
    hidden_blocks = hidden.astype(jnp.float32).reshape(row_count, N_TP, unit_count // N_TP)
    down_blocks = down_weight.astype(jnp.float32).reshape(N_TP, unit_count // N_TP, down_weight.shape[1])
    partial_value = jnp.einsum('rpf,pfd->prd', hidden_blocks, down_blocks).astype(jnp.bfloat16)
    return lax.optimization_barrier(jnp.sum(partial_value.astype(jnp.float32), 0))

def reference(hidden_in, mix_gain, w_query, w_key, w_value, w_outgate, w_gates, gate_bias, state_matrix, state_norm, state_max, w_mix_out, ffn_gain, routes, route_weights, expert_gate, expert_up, expert_down, shared_gate, shared_up, shared_down):
    normed = rms_scale(hidden_in, mix_gain).astype(jnp.bfloat16)

    def project(weight):
        rounded = jnp.dot(normed, weight, preferred_element_type=jnp.float32).astype(jnp.bfloat16)
        rounded = lax.optimization_barrier(rounded)
        return rounded.astype(jnp.float32).reshape(BATCH, HEADS, HEAD_DIM)
    query_heads = project(w_query)
    key_heads = project(w_key) * HEAD_DIM ** (-0.5)
    value_heads = project(w_value)
    out_gate = project(w_outgate)
    gate_pre = jnp.einsum('sd,gdh->gsh', normed.astype(jnp.float32), w_gates.astype(jnp.float32))
    gate_pre = gate_pre + gate_bias[:, None, :]
    carried = jax.nn.log_sigmoid(gate_pre[1]) + state_max
    new_max = jnp.maximum(carried, gate_pre[0])
    forget_weight = jnp.exp(carried - new_max)[..., None]
    input_weight = jnp.exp(gate_pre[0] - new_max)[..., None]
    new_norm = forget_weight * state_norm + input_weight * key_heads
    new_matrix = forget_weight[..., None] * state_matrix + (input_weight * value_heads)[..., :, None] * key_heads[..., None, :]
    numerator = jnp.einsum('shek,shk->she', new_matrix, query_heads, precision=lax.Precision.HIGHEST)
    denominator = jnp.maximum(jnp.abs(lax.optimization_barrier(jnp.sum(new_norm * query_heads, -1))), 1.0)
    gated_out = (jax.nn.sigmoid(out_gate) * numerator / denominator[..., None]).reshape(BATCH, M_WIDTH)
    gated_out = gated_out.astype(jnp.bfloat16)
    stream = (hidden_in.astype(jnp.float32) + jnp.dot(gated_out, w_mix_out, preferred_element_type=jnp.float32)).astype(jnp.bfloat16)
    ffn_in = rms_scale(stream, ffn_gain).astype(jnp.bfloat16)
    shared_hidden = (jax.nn.silu(jnp.dot(ffn_in, shared_gate, preferred_element_type=jnp.float32)) * jnp.dot(ffn_in, shared_up, preferred_element_type=jnp.float32)).astype(jnp.bfloat16)
    shared_out = block_sum(shared_hidden, shared_down)
    grouped = routes.reshape(N_EP, SEQ_GRP * TOP)
    onehot = (grouped[..., None] == jnp.arange(EXPERTS, dtype=jnp.int32)[None, None, :]).astype(jnp.int32)
    earlier = jnp.cumsum(onehot, 1) - onehot
    rank_counts = lax.optimization_barrier(jnp.sum(earlier * onehot, -1))
    group_ids = jnp.arange(N_EP, dtype=jnp.int32)[:, None]
    slot_ids = (grouped * (N_EP * CAP) + group_ids * CAP + rank_counts).reshape(-1).astype(jnp.int32)
    token_ids = (jnp.arange(BATCH * TOP, dtype=jnp.int32) // TOP).astype(jnp.int32)
    slot_tokens = jnp.full((EXPERTS * N_EP * CAP,), BATCH, jnp.int32).at[slot_ids].set(token_ids)
    padded_in = jnp.concatenate([ffn_in, jnp.zeros((1, D), jnp.bfloat16)], 0)

    def run_expert(operands):
        slot_picks, gate_weight, up_weight, down_weight = operands
        rows_in = padded_in[slot_picks]
        hidden = (jax.nn.silu(jnp.dot(rows_in, gate_weight, preferred_element_type=jnp.float32)) * jnp.dot(rows_in, up_weight, preferred_element_type=jnp.float32)).astype(jnp.bfloat16)
        return block_sum(hidden, down_weight).astype(jnp.bfloat16)
    expert_rows = lax.map(run_expert, (slot_tokens.reshape(EXPERTS, N_EP * CAP), expert_gate, expert_up, expert_down))
    flat_rows = expert_rows.reshape(EXPERTS * N_EP * CAP, D)
    picked = flat_rows[slot_ids].astype(jnp.float32).reshape(BATCH, TOP, D)
    routed = lax.optimization_barrier(jnp.sum(route_weights[..., None] * picked, 1))
    result = (stream.astype(jnp.float32) + shared_out + routed).astype(jnp.bfloat16)
    return (result, new_matrix, new_norm, new_max)
```

```python
import functools

import jax
import jax.numpy as jnp
from jax import lax
from jax.experimental import pallas as pl
from jax.experimental.pallas import tpu as pltpu
from jax.sharding import PartitionSpec as P

norm_eps = 1e-06


def rms_scale(inputs, scales):
    floats = inputs.astype(jnp.float32)
    return floats * lax.rsqrt(jnp.mean(floats * floats, -1, keepdims=True) + norm_eps) * scales


def swapped(block, axis, distance):
    count = lax.axis_size(axis)
    return lax.ppermute(block, axis, [(source, source ^ distance) for source in range(count)])


def columns_at(array, index, width):
    return lax.dynamic_slice_in_dim(array, index * width, width, 1)


def wide(array):
    return array.astype(jnp.float32)


def feed_forward(core_index, tokens, weights, slice_width, capacity):
    own_half, rows_half, gain = tokens[0], tokens[2], tokens[4]
    expert_gate, shared_gate = weights[0], weights[3]
    experts, width, hidden = expert_gate.shape
    shared_hidden = shared_gate.shape[1]
    own_count, routed_count = own_half.shape[0], rows_half.shape[0]
    row_count = own_count + routed_count
    half_width = width // 2
    chips = half_width // slice_width
    chunks = 4
    depth = width // chunks
    f32, bf16 = jnp.float32, jnp.bfloat16

    def kernel(
        core, own, own_other, routed, routed_other, gain,
        gate_far, up_far, down_far, sgate_far, sup_far, sdown_far,
        mine, theirs,
        gate, up, down, sgate, sup, sdown, inputs, sems,
    ):
        copies = []

        def fetch(source, target):
            copy = pltpu.make_async_copy(source, target, sems.at[len(copies)])
            copy.start()
            copies.append(copy)
            return copy

        chunk_copies = []
        for chunk in range(chunks):
            part = pl.ds(chunk * depth, depth)
            group = []
            for expert in range(experts):
                group.append(fetch(gate_far.at[expert, part], gate.at[expert, part]))
                group.append(fetch(up_far.at[expert, part], up.at[expert, part]))
            group.append(fetch(sgate_far.at[part], sgate.at[part]))
            group.append(fetch(sup_far.at[part], sup.at[part]))
            chunk_copies.append(group)
        down_copies = [fetch(down_far.at[expert], down.at[expert]) for expert in range(experts)]
        down_copies.append(fetch(sdown_far, sdown))

        first_core = core[0] == 0
        for first, other, start in ((own, own_other, 0), (routed, routed_other, own_count)):
            rows = first.shape[0]
            mass = jnp.zeros((rows, 1), f32)
            for chip in range(chips):
                columns = pl.ds(chip * slice_width, slice_width)
                for part in (first, other):
                    value = part[:, columns].astype(f32)
                    mass = mass + jnp.sum(value * value, -1, keepdims=True)
            scale = lax.rsqrt(mass / width + norm_eps)
            for chip in range(chips):
                columns = pl.ds(chip * slice_width, slice_width)
                one, two = first[:, columns].astype(f32), other[:, columns].astype(f32)
                pair = (jnp.where(first_core, one, two), jnp.where(first_core, two, one))
                for parity in range(2):
                    place = pl.ds((2 * chip + parity) * slice_width, slice_width)
                    fed = pair[parity] * scale * gain[:, place]
                    inputs[pl.ds(start, rows), place] = fed.astype(bf16)

        dot = functools.partial(jnp.dot, preferred_element_type=f32)
        gates = [jnp.zeros((routed_count, hidden), f32) for _ in range(experts)]
        ups = [jnp.zeros((routed_count, hidden), f32) for _ in range(experts)]
        own_gate = jnp.zeros((own_count, shared_hidden), f32)
        own_up = jnp.zeros((own_count, shared_hidden), f32)
        for chunk in range(chunks):
            part = pl.ds(chunk * depth, depth)
            for copy in chunk_copies[chunk]:
                copy.wait()
            routed_rows = inputs[pl.ds(own_count, routed_count), part]
            own_rows = inputs[pl.ds(0, own_count), part]
            for expert in range(experts):
                gates[expert] += dot(routed_rows, gate[expert, part, :])
                ups[expert] += dot(routed_rows, up[expert, part, :])
            own_gate += dot(own_rows, sgate[part, :])
            own_up += dot(own_rows, sup[part, :])
        row_ids = lax.broadcasted_iota(jnp.int32, (routed_count, hidden), 0)
        row_expert = row_ids % (experts * capacity) // capacity
        hiddens = []
        for expert in range(experts):
            value = gates[expert] / (1.0 + jnp.exp(-gates[expert])) * ups[expert]
            hiddens.append(jnp.where(row_expert == expert, value, 0.0).astype(bf16))
        own_hidden = (own_gate / (1.0 + jnp.exp(-own_gate)) * own_up).astype(bf16)
        for copy in down_copies:
            copy.wait()
        for chip in range(chips):
            pair = []
            for parity in range(2):
                place = pl.ds((2 * chip + parity) * slice_width, slice_width)
                total = dot(hiddens[0], down[0, :, place])
                for expert in range(1, experts):
                    total = total + dot(hiddens[expert], down[expert, :, place])
                pair.append((dot(own_hidden, sdown[:, place]), total))
            columns = pl.ds(chip * slice_width, slice_width)
            for index, start, rows in ((0, 0, own_count), (1, own_count, routed_count)):
                one, two = pair[0][index], pair[1][index]
                spot = pl.ds(start, rows)
                mine[spot, columns] = jnp.where(first_core, one, two).astype(bf16)
                theirs[spot, columns] = jnp.where(first_core, two, one).astype(bf16)

    near = pl.BlockSpec(memory_space=pltpu.VMEM)
    far = pl.BlockSpec(memory_space=pl.ANY)
    out = jax.ShapeDtypeStruct((row_count, half_width), bf16)
    copies = chunks * (2 * experts + 2) + experts + 1
    scratch = [pltpu.VMEM(weight.shape, bf16) for weight in weights]
    scratch += [pltpu.VMEM((row_count, width), bf16), pltpu.SemaphoreType.DMA((copies,))]
    return pl.pallas_call(
        kernel,
        out_shape=(out, out),
        in_specs=[pl.BlockSpec(memory_space=pltpu.SMEM)] + [near] * 5 + [far] * 6,
        out_specs=(near, near),
        scratch_shapes=scratch,
        compiler_params=pltpu.CompilerParams(vmem_limit_bytes=58 * 1024 * 1024),
        name="feed_forward",
    )(core_index, *tokens, *weights)


def per_device(
    hidden_in,
    mix_gain,
    w_query,
    w_key,
    w_value,
    w_outgate,
    w_gates,
    gate_bias,
    state_matrix,
    state_norm,
    state_max,
    w_mix_out,
    ffn_gain,
    routes,
    route_weights,
    expert_gate,
    expert_up,
    expert_down,
    shared_gate,
    shared_up,
    shared_down,
):
    ep_count = lax.axis_size("ep")
    tp_count = lax.axis_size("tp")
    group_index = lax.axis_index("ep")
    column_index = lax.axis_index("tp")
    core_index = column_index % 2
    chip_index = column_index // 2
    chip_count = tp_count // 2
    seq_rows, width = hidden_in.shape
    heads_dev = state_matrix.shape[1]
    head_dim = state_matrix.shape[2]
    top_count = routes.shape[1]
    local_experts = expert_gate.shape[0]
    expert_total = local_experts * ep_count
    capacity = max(2, seq_rows * top_count // expert_total + 1)
    group_slots = local_experts * capacity
    slice_width = width // tp_count
    half_width = width // 2
    feed_width = w_query.shape[0]
    bf16 = jnp.bfloat16
    floats = functools.partial(jnp.dot, preferred_element_type=jnp.float32)

    fed = [columns_at(hidden_in, group_index, feed_width)]
    for distance in range(1, ep_count):
        fed.append(
            swapped(columns_at(hidden_in, group_index ^ distance, feed_width), "ep", distance)
        )
    hidden_wide = wide(hidden_in)
    row_scale = lax.rsqrt(jnp.mean(hidden_wide * hidden_wide, -1, keepdims=True) + norm_eps)
    normed = (hidden_wide * row_scale * mix_gain).astype(bf16)
    gate_pre = jnp.einsum("sd,gdh->gsh", normed, w_gates, preferred_element_type=jnp.float32)
    gate_pre = gate_pre + gate_bias[:, None, :]
    carried = jax.nn.log_sigmoid(gate_pre[1]) + state_max
    new_max = jnp.maximum(carried, gate_pre[0])
    forget_weight = jnp.exp(carried - new_max)[..., None]
    input_weight = jnp.exp(gate_pre[0] - new_max)[..., None]

    feed_gain = lax.dynamic_slice_in_dim(mix_gain, group_index * feed_width, feed_width, 0)
    fed = jnp.concatenate(fed, 0)
    fed = (wide(fed) * feed_gain).astype(bf16)
    joined = jnp.concatenate([w_query, w_key, w_value, w_outgate], 1)
    partial = floats(fed, joined).astype(bf16)
    projected = wide(partial[:seq_rows])
    for distance in range(1, ep_count):
        block = partial[distance * seq_rows : (distance + 1) * seq_rows]
        projected = projected + wide(swapped(block, "ep", distance))
    projected = (projected * row_scale).astype(bf16)
    head_cols = heads_dev * head_dim

    def heads_of(role_index):
        part = projected[:, role_index * head_cols : (role_index + 1) * head_cols]
        return part.astype(jnp.float32).reshape(seq_rows, heads_dev, head_dim)

    query_heads = heads_of(0)
    key_heads = heads_of(1) * head_dim ** (-0.5)
    value_heads = heads_of(2)
    out_gate = heads_of(3)
    new_norm = forget_weight * state_norm + input_weight * key_heads
    new_matrix = (
        forget_weight[..., None] * state_matrix
        + (input_weight * value_heads)[..., :, None] * key_heads[..., None, :]
    )
    recalled = jnp.einsum(
        "shek,shk->she", state_matrix, query_heads, precision=lax.Precision.HIGHEST
    )
    matched = jnp.sum(key_heads * query_heads, -1, keepdims=True)
    numerator = forget_weight * recalled + input_weight * value_heads * matched
    denominator = jnp.maximum(jnp.abs(jnp.sum(new_norm * query_heads, -1)), 1.0)
    gated_out = (jax.nn.sigmoid(out_gate) * numerator / denominator[..., None]).reshape(
        seq_rows, head_cols
    )
    gated_out = gated_out.astype(bf16)

    def core_halves(array):
        cut = array.reshape(array.shape[0], chip_count, 2, slice_width)
        mine = lax.dynamic_index_in_dim(cut, core_index, 2, False)
        theirs = lax.dynamic_index_in_dim(cut, 1 - core_index, 2, False)
        flat = (array.shape[0], half_width)
        return mine.reshape(flat), theirs.reshape(flat)

    def chip_sum(array):
        mine, theirs = core_halves(array.astype(bf16))
        return wide(mine) + wide(swapped(theirs, "tp", 1))

    def chip_scatter(array):
        total = wide(columns_at(array, chip_index, slice_width))
        for distance in range(1, chip_count):
            block = columns_at(array, chip_index ^ distance, slice_width)
            total = total + wide(swapped(block, "tp", 2 * distance))
        return total

    mixed_half = chip_sum(floats(gated_out, w_mix_out)).astype(bf16)
    mixed_own = chip_scatter(mixed_half)
    residual_own = columns_at(hidden_in, column_index, slice_width)
    stream_own = (wide(residual_own) + mixed_own).astype(bf16)

    own_routes = lax.dynamic_slice_in_dim(routes, group_index * seq_rows, seq_rows, 0)
    places = jnp.arange(ep_count * group_slots, dtype=jnp.int32)
    place_group = (places // group_slots) ^ group_index
    place_expert = place_group * local_experts + places % group_slots // capacity
    named = own_routes[:, :, None] == place_expert[None, None, :]
    named_any = jnp.any(named, 1)
    before = jnp.arange(seq_rows)[:, None] > jnp.arange(seq_rows)[None, :]
    ranks = floats(before.astype(bf16), named_any.astype(bf16))
    chosen = named_any & (ranks == (places % capacity).astype(jnp.float32)[None, :])
    weights = jnp.sum(jnp.where(named, route_weights[:, :, None], 0.0), 1)
    weights = jnp.where(chosen, weights, 0.0)
    chooser = chosen.astype(bf16).T

    pieces = [stream_own]
    for distance in range(1, chip_count):
        pieces.append(swapped(stream_own, "tp", 2 * distance))
    stream_half = jnp.concatenate(
        [pick_chip(pieces, chip_index ^ place) for place in range(chip_count)], 1
    )
    arrived = []
    for distance in range(ep_count):
        block_chooser = chooser[distance * group_slots : (distance + 1) * group_slots]
        block = floats(block_chooser, stream_half).astype(bf16)
        arrived.append(swapped(block, "ep", distance) if distance else block)
    own_half = stream_half
    rows_half = jnp.concatenate(arrived, 0)

    own_other = swapped(own_half, "tp", 1)
    rows_other = swapped(rows_half, "tp", 1)
    mine, theirs = feed_forward(
        core_index.reshape(1).astype(jnp.int32),
        (own_half, own_other, rows_half, rows_other, ffn_gain.reshape(1, width)),
        (expert_gate, expert_up, expert_down, shared_gate, shared_up, shared_down),
        slice_width,
        capacity,
    )
    chip_part = wide(mine) + wide(swapped(theirs, "tp", 1))
    shared_half = chip_part[:seq_rows]
    routed_half = chip_part[seq_rows:].astype(bf16)
    returned = []
    for distance in range(ep_count):
        block = routed_half[distance * group_slots : (distance + 1) * group_slots]
        returned.append(swapped(block, "ep", distance) if distance else block)
    returned = jnp.concatenate(returned, 0)
    routed = jnp.dot(weights, wide(returned), precision=lax.Precision.HIGHEST)
    added_own = chip_scatter((routed + shared_half).astype(bf16))
    result = (wide(stream_own) + added_own).astype(bf16)
    return (result, new_matrix, new_norm, new_max)


def pick_chip(pieces, place):
    chosen = pieces[0]
    for distance in range(1, len(pieces)):
        chosen = jnp.where(place == distance, pieces[distance], chosen)
    return chosen


def solution(mesh):
    placed = (
        P("ep", None),
        P(),
        P("ep", "tp"),
        P("ep", "tp"),
        P("ep", "tp"),
        P("ep", "tp"),
        P(None, None, "tp"),
        P(None, "tp"),
        P("ep", "tp", None, None),
        P("ep", "tp", None),
        P("ep", "tp"),
        P("tp", None),
        P(),
        P(),
        P("ep", None),
        P("ep", None, "tp"),
        P("ep", None, "tp"),
        P("ep", "tp", None),
        P(None, "tp"),
        P(None, "tp"),
        P("tp", None),
    )
    return jax.shard_map(
        per_device,
        mesh=mesh,
        in_specs=placed,
        out_specs=(P("ep", "tp"), P("ep", "tp", None, None), P("ep", "tp", None), P("ep", "tp")),
        check_vma=False,
    )
```
